32 devices in a mesh: fs: 16 (over z, y, x), tp: 2 (over core).
Axes of the slice: x: 2, y: 2, z: 4, core: 2. Of those that a mesh axis runs over, the one named last changes fastest.
Arguments:
- tokens: bfloat16 [12288, 2048], P('fs'), may hold values from -6 to 6
- norm_gain: float32 [2048], replicated, may hold values from 0.1 to 1.9
- gate_weight: float32 [2048, 5120], P('fs', 'tp'), may hold values from -0.125 to 0.125
- value_weight: float32 [2048, 5120], P('fs', 'tp'), may hold values from -0.125 to 0.125
- gate_scale: float32 [5120], P('tp'), may hold values from 0.3 to 3
- value_scale: float32 [5120], P('tp'), may hold values from 0.3 to 3
- gate_kernel: float32 [3, 5120], P(None, 'tp'), may hold values from -3.5 to 3.5
- value_kernel: float32 [3, 5120], P(None, 'tp'), may hold values from -3.5 to 3.5
- gate_bias: float32 [5120], P('tp'), may hold values from -3 to 3
- value_bias: float32 [5120], P('tp'), may hold values from -3 to 3
- down_weight: float32 [5120, 2048], P('tp', 'fs'), may hold values from -0.078125 to 0.078125
- down_scale: float32 [2048], P('tp'), may hold values from 0.3 to 3
Outputs:
- mixed: bfloat16 [12288, 2048], P('fs', 'tp')
The draws below stay inside these ranges and needn't reach their ends.
All inputs are finite; a program needn't handle non-finite values.
Results may differ from the reference program's by a relative error of at most 0.014.
Values may be sent and summed in bfloat16 or wider, within the bound.
A program may use at most 128 MiB of HBM per device.

```python
import math
import jax
import jax.numpy as jnp
from jax import lax

D = 2048
FF = 5120
KERNEL = 3
TOK = 768
TOKENS = 12288
N_FS = 16
N_TP = 2


def block_scale(own_key, extent, shards, least, high):
    loudness, own = 1.0, jax.random.fold_in(own_key, 6)
    for dim, shards_of in shards:
        draws = jnp.exp(jax.random.uniform(jax.random.fold_in(own, dim), (shards_of,), jnp.float32, least / len(shards), high / len(shards)))
        loudness = loudness * jnp.repeat(draws, extent[dim] // shards_of).reshape([-1 if axis == dim else 1 for axis in range(len(extent))])
    return loudness


def gaussian(rng, extent, scale, most, cuts=(), held_as=jnp.bfloat16):
    level = block_scale(rng, extent, cuts, -0.22, 0.18) if cuts else 1.0
    entries = jax.random.normal(rng, extent, jnp.float32) * scale * level
    return jnp.minimum(jnp.maximum(entries, -most), most).astype(held_as)


def setup_inputs(seed: int = 0) -> dict:
    keys = jax.random.split(jax.random.key(seed), 13)
    return {
        "tokens": gaussian(keys[0], (TOKENS, D), 1.0, 6.0, ((0, 16),)),
        "norm_gain": jnp.clip(1.0 + 0.18 * jax.random.normal(keys[1], (D,), jnp.float32), 0.1, 1.9),
        "gate_weight": gaussian(keys[2], (D, FF), D ** -0.5, 0.125, ((0, 16), (1, 2)), jnp.float32),
        "value_weight": gaussian(keys[3], (D, FF), D ** -0.5, 0.125, ((0, 16), (1, 2)), jnp.float32),
        "gate_scale": jnp.clip(jnp.exp(math.log(3.0) - 2.3025851 * jax.random.uniform(keys[4], (FF,), jnp.float32) ** block_scale(keys[4], (FF,), ((0, 2),), -0.2, 0.2)), 0.3, 3.0),
        "value_scale": jnp.clip(jnp.exp(math.log(3.0) - 2.3025851 * jax.random.uniform(keys[5], (FF,), jnp.float32) ** block_scale(keys[5], (FF,), ((0, 2),), -0.2, 0.2)), 0.3, 3.0),
        "gate_kernel": gaussian(keys[6], (KERNEL, FF), KERNEL ** -0.5, 3.5, ((1, 2),), jnp.float32),
        "value_kernel": gaussian(keys[7], (KERNEL, FF), KERNEL ** -0.5, 3.5, ((1, 2),), jnp.float32),
        "gate_bias": gaussian(keys[8], (FF,), 0.5, 3.0, ((0, 2),), jnp.float32),
        "value_bias": gaussian(keys[9], (FF,), 0.5, 3.0, ((0, 2),), jnp.float32),
        "down_weight": gaussian(keys[10], (FF, D), FF ** -0.5, 0.078125, ((0, 2), (1, 16)), jnp.float32),
        "down_scale": jnp.clip(jnp.exp(math.log(3.0) - 2.3025851 * jax.random.uniform(keys[11], (D,), jnp.float32) ** block_scale(keys[11], (D,), ((0, 2),), -0.2, 0.2)), 0.3, 3.0),
    }


epsilon = 1e-06

def normalize(tokens, norm_gain):
    values = tokens.astype(jnp.float32)
    scaled = values * lax.rsqrt(lax.optimization_barrier(jnp.mean(values * values, axis=1, keepdims=True)) + epsilon)
    return (scaled * norm_gain[None, :]).astype(jnp.bfloat16)

def causal_mix(current, previous, kernel, tap_bias):
    row_count = current.shape[0]
    joined = jnp.concatenate([previous, current], axis=0).astype(jnp.float32)
    summed_taps = tap_bias[None, :] + kernel[2][None, :] * joined[2:]
    for back_by in (1, 2):
        summed_taps = summed_taps + kernel[2 - back_by][None, :] * joined[2 - back_by:2 - back_by + row_count]
    return summed_taps

def reference(tokens, norm_gain, gate_weight, value_weight, gate_scale, value_scale, gate_kernel, value_kernel, gate_bias, value_bias, down_weight, down_scale):
    gate_low = gate_weight.astype(jnp.bfloat16)
    value_low = value_weight.astype(jnp.bfloat16)
    down_low = down_weight.astype(jnp.bfloat16)
    block_width = FF // N_TP

    def one_block(carry, block_rows):
        previous_gate, previous_value = carry
        normed = normalize(block_rows, norm_gain)
        gate_pre = (jnp.dot(normed, gate_low, preferred_element_type=jnp.float32) * gate_scale[None, :]).astype(jnp.bfloat16)
        value_pre = (jnp.dot(normed, value_low, preferred_element_type=jnp.float32) * value_scale[None, :]).astype(jnp.bfloat16)
        gate_conv = causal_mix(gate_pre, previous_gate, gate_kernel, gate_bias)
        value_conv = causal_mix(value_pre, previous_value, value_kernel, value_bias)
        hidden = (jax.nn.gelu(gate_conv, approximate=True) * value_conv).astype(jnp.bfloat16)
        summed = jnp.zeros((block_rows.shape[0], D), jnp.float32)
        for block_index in range(N_TP):
            first_col = block_index * block_width
            partial_term = jnp.dot(hidden[:, first_col:first_col + block_width], down_low[first_col:first_col + block_width], preferred_element_type=jnp.float32).astype(jnp.bfloat16)
            partial_term = lax.optimization_barrier(partial_term)
            summed = summed + partial_term.astype(jnp.float32)
        result = (summed * down_scale[None, :]).astype(jnp.bfloat16)
        return ((gate_pre[-2:], value_pre[-2:]), result)
    start = (jnp.zeros((2, FF), jnp.bfloat16), jnp.zeros((2, FF), jnp.bfloat16))
    final_carry, mixed = lax.scan(one_block, start, tokens.reshape(N_FS, TOK, D))
    return mixed.reshape(TOKENS, D)
```

```python
import functools
import math

import jax
import jax.numpy as jnp
from jax import lax
from jax.experimental import pallas as pl
from jax.experimental.pallas import tpu as pltpu
from jax.sharding import PartitionSpec as P

epsilon = 1e-06


def from_behind(value, axis, steps):
    count = lax.axis_size(axis)
    leading, last = (max(0, -steps), min(count, count - steps))
    return lax.ppermute(value, axis, [(source, source + steps) for source in range(leading, last)])


def normalize(tokens, norm_gain):
    values = tokens.astype(jnp.float32)
    scaled = values * lax.rsqrt(jnp.mean(values * values, axis=1, keepdims=True) + epsilon)
    return (scaled * norm_gain[None, :]).astype(jnp.bfloat16)


def causal_mix(current, previous, kernel, tap_bias):
    row_count = current.shape[0]
    joined = jnp.concatenate([previous, current], axis=0).astype(jnp.float32)
    summed_taps = tap_bias[None, :] + kernel[2][None, :] * joined[2:]
    for back_by in (1, 2):
        summed_taps = (
            summed_taps
            + kernel[2 - back_by][None, :] * joined[2 - back_by : 2 - back_by + row_count]
        )
    return summed_taps


def body(
    tokens,
    norm_gain,
    gate_weight,
    value_weight,
    gate_scale,
    value_scale,
    gate_kernel,
    value_kernel,
    gate_bias,
    value_bias,
    down_weight,
    down_scale,
):
    normed = normalize(tokens, norm_gain)
    gate_low = gate_weight.astype(jnp.bfloat16)
    value_low = value_weight.astype(jnp.bfloat16)
    down_low = down_weight.astype(jnp.bfloat16)
    row_count = normed.shape[0]
    gate_full, value_full, down_full = (
        lax.all_gather(gate_low, "fs", axis=0, tiled=True),
        lax.all_gather(value_low, "fs", axis=0, tiled=True),
        lax.all_gather(down_low, "fs", axis=1, tiled=True),
    )
    gate_raw = jnp.dot(normed, gate_full, preferred_element_type=jnp.float32)
    value_raw = jnp.dot(normed, value_full, preferred_element_type=jnp.float32)
    gate_pre = (gate_raw * gate_scale[None, :]).astype(jnp.bfloat16)
    value_pre = (value_raw * value_scale[None, :]).astype(jnp.bfloat16)
    previous_gate, previous_value = from_behind(
        (gate_pre[row_count - 2 :], value_pre[row_count - 2 :]), "fs", 1
    )
    gate_conv = causal_mix(gate_pre, previous_gate, gate_kernel, gate_bias)
    value_conv = causal_mix(value_pre, previous_value, value_kernel, value_bias)
    hidden = (jax.nn.gelu(gate_conv, approximate=True) * value_conv).astype(jnp.bfloat16)
    partial_terms = jnp.dot(hidden, down_full, preferred_element_type=jnp.float32)
    summed = lax.psum_scatter(
        partial_terms.astype(jnp.bfloat16), "tp", scatter_dimension=1, tiled=True
    ).astype(jnp.float32)
    return (summed * down_scale[None, :]).astype(jnp.bfloat16)


MESH = pl.DeviceIdType.MESH
GROUP = 4


def fused_kernel(
    depth_planes,
    nrm,
    wu,
    wd,
    par,
    osc,
    out,
    tok,
    up_all,
    down_all,
    hidden,
    stage,
    pair_in,
    peer_in,
    taps,
    halo_out,
    halo_in,
    sem_local,
    sem_plane_send,
    sem_up_recv,
    sem_down_recv,
    sem_up_send,
    sem_down_send,
    sem_tok_send,
    sem_tok_recv,
    sem_tok_pair_send,
    sem_tok_pair_recv,
    sem_halo,
    sem_pair_send,
    sem_pair_recv,
    sem_peer_send,
    sem_peer_recv,
):
    planes = depth_planes
    half = planes // 2
    me = lax.axis_index("fs")
    core = lax.axis_index("tp")
    z, p = me // GROUP, me % GROUP
    rows_own = nrm.shape[0]
    part_rows = rows_own // 2
    piece = wu.shape[1]
    units = hidden.shape[1]
    out_piece = wd.shape[2]
    chunk = GROUP * out_piece
    has_up, has_down = z < planes - 1, z > 0

    def flip(mask):
        px, py = p % 2, p // 2
        if mask & 1:
            px = 1 - px
        if mask & 2:
            py = 1 - py
        return py * 2 + px

    def chip(target):
        return (z * GROUP + target, core)

    others = (1, 2, 3)

    barrier = pltpu.get_barrier_semaphore()
    for mask in others:
        pl.semaphore_signal(barrier, inc=1, device_id=chip(flip(mask)), device_id_type=MESH)
    pl.semaphore_signal(barrier, inc=1, device_id=(me, 1 - core), device_id_type=MESH)

    @pl.when(has_up)
    def _():
        pl.semaphore_signal(barrier, inc=1, device_id=(me + GROUP, core), device_id_type=MESH)

    @pl.when(has_down)
    def _():
        pl.semaphore_signal(barrier, inc=1, device_id=(me - GROUP, core), device_id_type=MESH)

    pl.semaphore_wait(barrier, 4 + has_up.astype(jnp.int32) + has_down.astype(jnp.int32))

    def up_block(f):
        return up_all.at[pl.ds(pl.multiple_of(f * piece, piece), piece), :]

    def down_block(f):
        return down_all.at[:, pl.ds(pl.multiple_of(f * out_piece, out_piece), out_piece)]

    def remote(src, dst, send, recv, device):
        return pltpu.make_async_remote_copy(
            src_ref=src, dst_ref=dst, send_sem=send, recv_sem=recv, device_id=device, device_id_type=MESH
        )

    def plane_copy(kind, mask):
        target = flip(mask)
        src, block, recv = ((wu, up_block, sem_up_recv), (wd, down_block, sem_down_recv))[kind]
        return remote(src.at[target], block(me), sem_plane_send.at[kind, mask], recv.at[me], chip(target))

    def line_copy(kind, direction, f):
        block, send, recv = (
            (up_block, sem_up_send, sem_up_recv),
            (down_block, sem_down_send, sem_down_recv),
        )[kind]
        step = GROUP if direction == 0 else -GROUP
        return remote(block(f), block(f), send.at[direction, f], recv.at[f], (me + step, core))

    def wait_piece(kind, f):
        block, send, recv = (
            (up_block, sem_up_send, sem_up_recv),
            (down_block, sem_down_send, sem_down_recv),
        )[kind]
        remote(block(f), block(f), send.at[0, f], recv.at[f], (me, 1 - core)).wait_recv()

    def forward(kind, direction, f):
        @pl.when(has_up if direction == 0 else has_down)
        def _():
            line_copy(kind, direction, f).start()

    def token_rows(owner, part):
        start = pl.multiple_of(owner * rows_own + part * part_rows, part_rows)
        return tok.at[pl.ds(start, part_rows), :]

    def token_copy(mask):
        start = pl.multiple_of(core * part_rows, part_rows)
        return remote(
            nrm.at[pl.ds(start, part_rows), :],
            token_rows(p, core),
            sem_tok_send.at[mask],
            sem_tok_recv.at[mask],
            chip(flip(mask)),
        )

    def token_pair_copy(mask):
        here = token_rows(flip(mask), core)
        return remote(here, here, sem_tok_pair_send.at[mask], sem_tok_pair_recv.at[mask], (me, 1 - core))

    own_up = pltpu.make_async_copy(wu.at[p], up_block(me), sem_local.at[0])
    own_down = pltpu.make_async_copy(wd.at[p], down_block(me), sem_local.at[1])
    own_tok = pltpu.make_async_copy(
        nrm, tok.at[pl.ds(pl.multiple_of(p * rows_own, rows_own), rows_own), :], sem_local.at[2]
    )
    own_up.start()
    own_down.start()
    own_tok.start()
    for kind in (0, 1):
        for mask in others:
            plane_copy(kind, mask).start()
    for mask in others:
        token_copy(mask).start()
    own_up.wait()
    for direction in (0, 1):
        forward(0, direction, me)
    own_down.wait()
    own_tok.wait()
    for mask in others:
        f = z * GROUP + flip(mask)
        wait_piece(0, f)
        for direction in (0, 1):
            forward(0, direction, f)

    def plane_of(step):
        distance = (step + 1) // 2
        below = step % 2
        return z + distance * (1 - 2 * below), below

    def relay(kind, q, below):
        def one(i, carry):
            f = q * GROUP + i
            wait_piece(kind, f)

            @pl.when((below == 1) & has_up)
            def _():
                line_copy(kind, 0, f).start()

            @pl.when((below == 0) & has_down)
            def _():
                line_copy(kind, 1, f).start()

            return carry

        lax.fori_loop(0, GROUP, one, 0)

    def up_step(step, carry):
        q, below = plane_of(step)

        @pl.when((q >= 0) & (q < planes))
        def _():
            relay(0, q, below)

        return carry

    lax.fori_loop(1, 2 * planes - 1, up_step, 0)

    for direction in (0, 1):
        forward(1, direction, me)
    for mask in others:
        f = z * GROUP + flip(mask)
        wait_piece(1, f)
        for direction in (0, 1):
            forward(1, direction, f)

    def token_pair_wait(mask):
        there = token_rows(flip(mask), 1 - core)
        remote(there, there, sem_tok_pair_send.at[mask], sem_tok_pair_recv.at[mask], (me, 1 - core)).wait_recv()

    for mask in others:
        landed = token_rows(flip(mask), core)
        remote(landed, landed, sem_tok_send.at[mask], sem_tok_recv.at[mask], (me, 1 - core)).wait_recv()
        token_pair_copy(mask).start()
    for mask in others:
        token_pair_wait(mask)

    all_rows = tok.shape[0]
    columns = up_all.shape[1]
    tile = taps.shape[0] - 8
    halo_rows = halo_out.shape[0]

    def wide(j):
        return pl.ds(pl.multiple_of(j * 256, 256), 256)

    def halo_step(j, carry):
        raw = jnp.dot(tok[all_rows - halo_rows :, :], up_all[:, wide(j)], preferred_element_type=jnp.float32)
        halo_out[:, wide(j)] = (raw * par[0:1, wide(j)]).astype(jnp.bfloat16)
        return carry

    lax.fori_loop(0, columns // 256, halo_step, 0)

    halo_copy = remote(halo_out, halo_in, sem_halo.at[0], sem_halo.at[1], (me + GROUP, core))

    @pl.when(has_up)
    def _():
        halo_copy.start()

    @pl.when(has_down)
    def _():
        remote(halo_out, halo_in, sem_halo.at[0], sem_halo.at[1], (me, 1 - core)).wait_recv()

    @pl.when(jnp.logical_not(has_down))
    def _():
        halo_in[...] = jnp.zeros_like(halo_in)

    def column_step(j, carry):
        taps[0:8, :] = halo_in[:, wide(j)].astype(jnp.float32)[halo_rows - 8 :, :]

        def row_step(m, inner):
            rows = pl.ds(pl.multiple_of(m * tile, tile), tile)
            raw = jnp.dot(tok[rows, :], up_all[:, wide(j)], preferred_element_type=jnp.float32)
            taps[8:, :] = (raw * par[0:1, wide(j)]).astype(jnp.bfloat16).astype(jnp.float32)
            conv = par[4:5, wide(j)] + par[3:4, wide(j)] * taps[8 : 8 + tile, :]
            conv = conv + par[2:3, wide(j)] * taps[7 : 7 + tile, :]
            conv = conv + par[1:2, wide(j)] * taps[6 : 6 + tile, :]
            g, v = conv[:, :128], conv[:, 128:]
            act = 0.5 * g * (1.0 + jnp.tanh(math.sqrt(2.0 / math.pi) * (g + 0.044715 * (g * g * g))))
            hidden[rows, pl.ds(pl.multiple_of(j * 128, 128), 128)] = (act * v).astype(jnp.bfloat16)
            taps[0:8, :] = taps[tile : tile + 8, :]
            return inner

        return lax.fori_loop(0, all_rows // tile, row_step, carry)

    lax.fori_loop(0, columns // 256, column_step, 0)

    def block_rows(owner):
        return pl.ds(pl.multiple_of(owner * rows_own, rows_own), rows_own)

    def pair_copy(q, owner):
        return remote(
            stage.at[q, owner],
            pair_in.at[q % half, owner],
            sem_pair_send.at[q % half, owner],
            sem_pair_recv.at[q % half, owner],
            (me, 1 - core),
        )

    def peer_copy(q, mask):
        return remote(
            stage.at[q, flip(mask)],
            peer_in.at[q % half, mask - 1],
            sem_peer_send.at[q % half, mask],
            sem_peer_recv.at[q % half, mask],
            chip(flip(mask)),
        )

    def down_step(step, carry):
        q, below = plane_of(step)

        @pl.when((q >= 0) & (q < planes))
        def _():
            @pl.when(step > 0)
            def _():
                relay(1, q, below)

            mine = q // half == core
            cols = pl.ds(pl.multiple_of(q * chunk, chunk), chunk)

            def product(owner, inner):
                value = jnp.dot(hidden[block_rows(owner), :], down_all[:, cols], preferred_element_type=jnp.float32)
                stage[q, owner] = value.astype(jnp.bfloat16)

                @pl.when(jnp.logical_not(mine))
                def _():
                    pair_copy(q, owner).start()

                return inner

            lax.fori_loop(0, GROUP, product, 0)

            @pl.when(mine)
            def _():
                def combine(owner):
                    pair_copy(q, owner).wait_recv()
                    both = stage[q, owner].astype(jnp.float32) + pair_in[q % half, owner].astype(jnp.float32)
                    stage[q, owner] = both.astype(jnp.bfloat16)

                for mask in (3, 1, 2):
                    combine(flip(mask))
                    peer_copy(q, mask).start()
                combine(p)

        return carry

    lax.fori_loop(0, 2 * planes - 1, down_step, 0)

    def finish(i, carry):
        q = core * half + i
        total = stage[q, p].astype(jnp.float32)
        for mask in others:
            peer_copy(q, mask).wait_recv()
            total = total + peer_in[i, mask - 1].astype(jnp.float32)
        cols = pl.ds(pl.multiple_of(i * chunk, chunk), chunk)
        out[:, cols] = (total * osc[0:1, cols]).astype(jnp.bfloat16)
        return carry

    lax.fori_loop(0, half, finish, 0)

    def drain_out(i, carry):
        for mask in others:
            peer_copy(core * half + i, mask).wait_send()

        def one(owner, inner):
            pair_copy((1 - core) * half + i, owner).wait_send()
            return inner

        return lax.fori_loop(0, GROUP, one, carry)

    lax.fori_loop(0, half, drain_out, 0)
    for mask in others:
        token_copy(mask).wait_send()
        token_pair_copy(mask).wait_send()
        for kind in (0, 1):
            plane_copy(kind, mask).wait_send()

    @pl.when(has_up)
    def _():
        halo_copy.wait_send()

    def drain_line(f, carry):
        for kind in (0, 1):

            @pl.when(has_up & (f // GROUP <= z))
            def _():
                line_copy(kind, 0, f).wait_send()

            @pl.when(has_down & (f // GROUP >= z))
            def _():
                line_copy(kind, 1, f).wait_send()

        return carry

    lax.fori_loop(0, planes * GROUP, drain_line, 0)


def grouped_body(count, tokens, norm_gain, gate_weight, value_weight, gate_scale, value_scale, gate_kernel, value_kernel, gate_bias, value_bias, down_weight, down_scale):
    planes = count // GROUP
    half = planes // 2
    p = lax.axis_index("fs") % GROUP
    normed = normalize(tokens, norm_gain)
    rows, width = normed.shape
    piece, local = gate_weight.shape
    out_piece = down_weight.shape[1]
    units = local // GROUP
    blocks = units // 128
    chunk = GROUP * out_piece
    both = jnp.stack([gate_weight.astype(jnp.bfloat16), value_weight.astype(jnp.bfloat16)], axis=0)
    both = both.reshape(2, piece, GROUP, blocks, 128).transpose(2, 1, 3, 0, 4)
    wu = both.reshape(GROUP, piece, 2 * units)
    wd = down_weight.astype(jnp.bfloat16).reshape(GROUP, units, out_piece)

    def pick(gate, value):
        gate = lax.dynamic_slice_in_dim(gate, p * units, units, axis=1)
        value = lax.dynamic_slice_in_dim(value, p * units, units, axis=1)
        n = gate.shape[0]
        pair = jnp.stack([gate.reshape(n, blocks, 128), value.reshape(n, blocks, 128)], axis=2)
        return pair.reshape(n, 2 * units)

    gate_rows = jnp.concatenate([gate_scale[None], gate_kernel, gate_bias[None], jnp.zeros((3, local), jnp.float32)], axis=0)
    value_rows = jnp.concatenate([value_scale[None], value_kernel, value_bias[None], jnp.zeros((3, local), jnp.float32)], axis=0)
    par = pick(gate_rows, value_rows)
    tile = rows // 2
    dma = pltpu.SemaphoreType.DMA
    bf16 = jnp.bfloat16
    vmem = pl.BlockSpec(memory_space=pltpu.VMEM)
    return pl.pallas_call(
        functools.partial(fused_kernel, planes),
        out_shape=jax.ShapeDtypeStruct((rows, half * chunk), bf16),
        in_specs=[vmem] * 5,
        out_specs=vmem,
        scratch_shapes=[
            pltpu.VMEM((GROUP * rows, width), bf16),
            pltpu.VMEM((width, 2 * units), bf16),
            pltpu.VMEM((units, width), bf16),
            pltpu.VMEM((GROUP * rows, units), bf16),
            pltpu.VMEM((planes, GROUP, rows, chunk), bf16),
            pltpu.VMEM((half, GROUP, rows, chunk), bf16),
            pltpu.VMEM((half, GROUP - 1, rows, chunk), bf16),
            pltpu.VMEM((tile + 8, 256), jnp.float32),
            pltpu.VMEM((16, 2 * units), bf16),
            pltpu.VMEM((16, 2 * units), bf16),
            dma((3,)),
            dma((2, GROUP)),
            dma((count,)),
            dma((count,)),
            dma((2, count)),
            dma((2, count)),
            dma((GROUP,)),
            dma((GROUP,)),
            dma((GROUP,)),
            dma((GROUP,)),
            dma((2,)),
            dma((half, GROUP)),
            dma((half, GROUP)),
            dma((half, GROUP)),
            dma((half, GROUP)),
        ],
        compiler_params=pltpu.CompilerParams(
            collective_id=0, has_side_effects=True, vmem_limit_bytes=67043328
        ),
    )(normed, wu, wd, par, down_scale[None, :])


def solution(mesh):
    count, tp = mesh.shape["fs"], mesh.shape["tp"]

    def whole(*arrays):
        local = arrays[2].shape[1]
        fits = tp == 2 and count % (2 * GROUP) == 0 and local % (GROUP * 128) == 0
        if fits:
            return grouped_body(count, *arrays)
        return body(*arrays)

    return jax.shard_map(
        whole,
        mesh=mesh,
        in_specs=(
            P("fs", None),
            P(),
            P("fs", "tp"),
            P("fs", "tp"),
            P("tp"),
            P("tp"),
            P(None, "tp"),
            P(None, "tp"),
            P("tp"),
            P("tp"),
            P("tp", "fs"),
            P("tp"),
        ),
        out_specs=P("fs", "tp"),
        check_vma=False,
    )
```

```python
import functools
import math

import jax
import jax.numpy as jnp
from jax import lax
from jax.experimental import pallas as pl
from jax.experimental.pallas import tpu as pltpu
from jax.sharding import PartitionSpec as P

epsilon = 1e-06


def from_behind(value, axis, steps):
    count = lax.axis_size(axis)
    leading, last = (max(0, -steps), min(count, count - steps))
    return lax.ppermute(value, axis, [(source, source + steps) for source in range(leading, last)])


def normalize(tokens, norm_gain):
    values = tokens.astype(jnp.float32)
    scaled = values * lax.rsqrt(jnp.mean(values * values, axis=1, keepdims=True) + epsilon)
    return (scaled * norm_gain[None, :]).astype(jnp.bfloat16)


def causal_mix(current, previous, kernel, tap_bias):
    row_count = current.shape[0]
    joined = jnp.concatenate([previous, current], axis=0).astype(jnp.float32)
    summed_taps = tap_bias[None, :] + kernel[2][None, :] * joined[2:]
    for back_by in (1, 2):
        summed_taps = (
            summed_taps
            + kernel[2 - back_by][None, :] * joined[2 - back_by : 2 - back_by + row_count]
        )
    return summed_taps


def body(
    tokens,
    norm_gain,
    gate_weight,
    value_weight,
    gate_scale,
    value_scale,
    gate_kernel,
    value_kernel,
    gate_bias,
    value_bias,
    down_weight,
    down_scale,
):
    normed = normalize(tokens, norm_gain)
    gate_low = gate_weight.astype(jnp.bfloat16)
    value_low = value_weight.astype(jnp.bfloat16)
    down_low = down_weight.astype(jnp.bfloat16)
    row_count = normed.shape[0]
    gate_full, value_full, down_full = (
        lax.all_gather(gate_low, "fs", axis=0, tiled=True),
        lax.all_gather(value_low, "fs", axis=0, tiled=True),
        lax.all_gather(down_low, "fs", axis=1, tiled=True),
    )
    gate_raw = jnp.dot(normed, gate_full, preferred_element_type=jnp.float32)
    value_raw = jnp.dot(normed, value_full, preferred_element_type=jnp.float32)
    gate_pre = (gate_raw * gate_scale[None, :]).astype(jnp.bfloat16)
    value_pre = (value_raw * value_scale[None, :]).astype(jnp.bfloat16)
    previous_gate, previous_value = from_behind(
        (gate_pre[row_count - 2 :], value_pre[row_count - 2 :]), "fs", 1
    )
    gate_conv = causal_mix(gate_pre, previous_gate, gate_kernel, gate_bias)
    value_conv = causal_mix(value_pre, previous_value, value_kernel, value_bias)
    hidden = (jax.nn.gelu(gate_conv, approximate=True) * value_conv).astype(jnp.bfloat16)
    partial_terms = jnp.dot(hidden, down_full, preferred_element_type=jnp.float32)
    summed = lax.psum_scatter(
        partial_terms.astype(jnp.bfloat16), "tp", scatter_dimension=1, tiled=True
    ).astype(jnp.float32)
    return (summed * down_scale[None, :]).astype(jnp.bfloat16)


MESH = pl.DeviceIdType.MESH
GROUP = 4


def fused_kernel(
    depth_planes,
    tok_hbm,
    gate_hbm,
    value_hbm,
    down_hbm,
    gain,
    gate_scale,
    value_scale,
    gate_kernel,
    value_kernel,
    gate_bias,
    value_bias,
    osc,
    out,
    tok,
    up_all,
    down_all,
    hidden,
    stage,
    pair_in,
    peer_in,
    relay_in,
    taps,
    halo_out,
    halo_in,
    par,
    wu,
    wd,
    raw_tok,
    raw_gate,
    raw_value,
    raw_down,
    sem_local,
    sem_plane_send,
    sem_up_recv,
    sem_down_recv,
    sem_up_send,
    sem_down_send,
    sem_tok_send,
    sem_tok_recv,
    sem_tok_pair_send,
    sem_tok_pair_recv,
    sem_halo,
    sem_pair_send,
    sem_pair_recv,
    sem_peer_send,
    sem_peer_recv,
    sem_relay_send,
    sem_relay_recv,
    sem_late_recv,
    sem_late_send,
):
    planes = depth_planes
    half = planes // 2
    me = lax.axis_index("fs")
    core = lax.axis_index("tp")
    z, p = me // GROUP, me % GROUP
    rows_own = raw_tok.shape[0]
    part_rows = rows_own // 2
    piece = wu.shape[1]
    units = hidden.shape[1]
    out_piece = wd.shape[2]
    chunk = GROUP * out_piece
    has_up, has_down = z < planes - 1, z > 0

    def flip(mask):
        px, py = p % 2, p // 2
        if mask & 1:
            px = 1 - px
        if mask & 2:
            py = 1 - py
        return py * 2 + px

    def chip(target):
        return (z * GROUP + target, core)

    others = (1, 2, 3)

    fetches = [
        pltpu.make_async_copy(src, dst, sem_local.at[2 + i])
        for i, (src, dst) in enumerate(
            ((gate_hbm, raw_gate), (value_hbm, raw_value), (down_hbm, raw_down), (tok_hbm, raw_tok))
        )
    ]
    for fetch in fetches:
        fetch.start()

    barrier = pltpu.get_barrier_semaphore()
    for mask in others:
        pl.semaphore_signal(barrier, inc=1, device_id=chip(flip(mask)), device_id_type=MESH)
    pl.semaphore_signal(barrier, inc=1, device_id=(me, 1 - core), device_id_type=MESH)

    @pl.when(has_up)
    def _():
        pl.semaphore_signal(barrier, inc=1, device_id=(me + GROUP, core), device_id_type=MESH)

    @pl.when(has_down)
    def _():
        pl.semaphore_signal(barrier, inc=1, device_id=(me - GROUP, core), device_id_type=MESH)

    blocks = units // 128
    fetches[0].wait()
    fetches[1].wait()
    for m in range(GROUP):
        for j in range(blocks):
            first = (m * blocks + j) * 128
            wu[m, :, j * 256 : j * 256 + 128] = raw_gate[:, first : first + 128].astype(jnp.bfloat16)
            wu[m, :, j * 256 + 128 : j * 256 + 256] = raw_value[:, first : first + 128].astype(jnp.bfloat16)
    fetches[2].wait()
    for m in range(GROUP):
        wd[m] = raw_down[m * units : (m + 1) * units, :].astype(jnp.bfloat16)
    for j in range(blocks):
        src = pl.ds(pl.multiple_of(p * units + j * 128, 128), 128)
        for side, (scale, kernel, tap_bias) in enumerate(
            ((gate_scale, gate_kernel, gate_bias), (value_scale, value_kernel, value_bias))
        ):
            dst = slice(j * 256 + side * 128, j * 256 + side * 128 + 128)
            par[0:1, dst] = scale[0:1, src]
            par[1:4, dst] = kernel[0:3, src]
            par[4:5, dst] = tap_bias[0:1, src]
    pl.semaphore_wait(barrier, 4 + has_up.astype(jnp.int32) + has_down.astype(jnp.int32))

    early = (blocks + 1) // 2 * 256
    columns = up_all.shape[1]

    def up_whole(f):
        return up_all.at[pl.ds(pl.multiple_of(f * piece, piece), piece), :]

    def up_block(f):
        return up_all.at[pl.ds(pl.multiple_of(f * piece, piece), piece), 0:early]

    def late_block(f):
        return up_all.at[pl.ds(pl.multiple_of(f * piece, piece), piece), early:columns]

    def down_block(f):
        return down_all.at[:, pl.ds(pl.multiple_of(f * out_piece, out_piece), out_piece)]

    kinds = (
        (up_block, sem_up_send, sem_up_recv),
        (down_block, sem_down_send, sem_down_recv),
        (late_block, sem_late_send, sem_late_recv),
    )

    def remote(src, dst, send, recv, device):
        return pltpu.make_async_remote_copy(
            src_ref=src, dst_ref=dst, send_sem=send, recv_sem=recv, device_id=device, device_id_type=MESH
        )

    def plane_copy(kind, mask):
        target = flip(mask)
        block, _, recv = kinds[kind]
        src = (wu.at[target, :, 0:early], wd.at[target], wu.at[target, :, early:columns])[kind]
        return remote(src, block(me), sem_plane_send.at[kind, mask], recv.at[me], chip(target))

    def line_copy(kind, direction, f):
        block, send, recv = kinds[kind]
        step = GROUP if direction == 0 else -GROUP
        return remote(block(f), block(f), send.at[direction, f], recv.at[f], (me + step, core))

    def wait_piece(kind, f):
        block, send, recv = kinds[kind]
        remote(block(f), block(f), send.at[0, f], recv.at[f], (me, 1 - core)).wait_recv()

    def forward(kind, direction, f):
        @pl.when(has_up if direction == 0 else has_down)
        def _():
            line_copy(kind, direction, f).start()

    def token_rows(owner, part):
        start = pl.multiple_of(owner * rows_own + part * part_rows, part_rows)
        return tok.at[pl.ds(start, part_rows), :]

    def token_copy(mask):
        here = token_rows(p, core)
        return remote(here, here, sem_tok_send.at[mask], sem_tok_recv.at[mask], chip(flip(mask)))

    quarter = part_rows // 2

    def token_quarter(owner, which):
        start = owner * rows_own + core * part_rows + which * quarter
        return tok.at[pl.ds(pl.multiple_of(start, quarter), quarter), :]

    def token_relay(mask):
        which = mask - 1
        slot = (3, 0)[which]
        here = token_quarter(flip(mask), which)
        return remote(here, here, sem_tok_send.at[slot], sem_tok_recv.at[slot], chip(flip(3 - mask)))

    def token_pair_copy(mask):
        here = token_rows(flip(mask), core)
        return remote(here, here, sem_tok_pair_send.at[mask], sem_tok_pair_recv.at[mask], (me, 1 - core))

    own_up = pltpu.make_async_copy(wu.at[p], up_whole(me), sem_local.at[0])
    own_down = pltpu.make_async_copy(wd.at[p], down_block(me), sem_local.at[1])
    own_up.start()
    own_down.start()
    for kind in (0, 2):
        for mask in others:
            plane_copy(kind, mask).start()
    own_up.wait()
    for direction in (0, 1):
        forward(0, direction, me)

    fetches[3].wait()
    norm_tile = 64

    def norm_step(i, carry):
        first = pl.multiple_of(i * norm_tile, norm_tile)
        values = raw_tok[pl.ds(first, norm_tile), :].astype(jnp.float32)
        scaled = values * lax.rsqrt(jnp.mean(values * values, axis=1, keepdims=True) + epsilon)
        rows = pl.ds(pl.multiple_of(p * rows_own + i * norm_tile, norm_tile), norm_tile)
        tok[rows, :] = (scaled * gain[...]).astype(jnp.bfloat16)
        return carry

    lax.fori_loop(0, rows_own // norm_tile, norm_step, 0)
    own_down.wait()

    def own_plane(kind):
        for mask in others:
            f = z * GROUP + flip(mask)
            wait_piece(kind, f)
            for direction in (0, 1):
                forward(kind, direction, f)

    own_plane(0)
    for mask in (1, 2):
        token_copy(mask).start()
    for mask in others:
        plane_copy(1, mask).start()
    for direction in (0, 1):
        forward(2, direction, me)
    own_plane(2)

    def plane_of(step):
        distance = (step + 1) // 2
        below = step % 2
        return z + distance * (1 - 2 * below), below

    def relay_one(kind, q, below, i):
        f = q * GROUP + i
        wait_piece(kind, f)

        @pl.when((below == 1) & has_up)
        def _():
            line_copy(kind, 0, f).start()

        @pl.when((below == 0) & has_down)
        def _():
            line_copy(kind, 1, f).start()

    def relay(kind, q, below):
        def one(i, carry):
            relay_one(kind, q, below, i)
            return carry

        lax.fori_loop(0, GROUP, one, 0)

    def up_step(step, carry):
        q, below = plane_of(step)

        @pl.when((q >= 0) & (q < planes))
        def _():
            relay(0, q, below)

        return carry

    lax.fori_loop(1, 2 * planes - 3, up_step, 0)

    def token_wait(mask):
        landed = token_rows(flip(mask), core)
        remote(landed, landed, sem_tok_send.at[mask], sem_tok_recv.at[mask], (me, 1 - core)).wait_recv()

    for mask in (1, 2):
        token_wait(mask)
        token_relay(mask).start()
        token_pair_copy(mask).start()

    lax.fori_loop(2 * planes - 3, 2 * planes - 1, up_step, 0)

    def token_pair_wait(mask):
        there = token_rows(flip(mask), 1 - core)
        remote(there, there, sem_tok_pair_send.at[mask], sem_tok_pair_recv.at[mask], (me, 1 - core)).wait_recv()

    for which in (0, 1):
        slot = (3, 0)[which]
        landed = token_quarter(flip(3), which)
        remote(landed, landed, sem_tok_send.at[slot], sem_tok_recv.at[slot], (me, 1 - core)).wait_recv()
    token_pair_copy(3).start()
    for mask in others:
        token_pair_wait(mask)

    all_rows = tok.shape[0]
    tile = taps.shape[0] - 8
    halo_rows = halo_out.shape[0]

    def wide(j):
        return pl.ds(pl.multiple_of(j * 256, 256), 256)

    def halo_step(j, carry):
        raw = jnp.dot(tok[all_rows - halo_rows :, :], up_all[:, wide(j)], preferred_element_type=jnp.float32)
        halo_out[:, wide(j)] = (raw * par[0:1, wide(j)]).astype(jnp.bfloat16)
        return carry

    def halo_copy(part):
        cols = (slice(0, early), slice(early, columns))[part]
        here, there = halo_out.at[:, cols], halo_in.at[:, cols]
        return remote(here, there, sem_halo.at[part], sem_halo.at[2 + part], (me + GROUP, core))

    def halo_part(part, first, last):
        lax.fori_loop(first, last, halo_step, 0)

        @pl.when(has_up)
        def _():
            halo_copy(part).start()

        @pl.when(has_down)
        def _():
            cols = (slice(0, early), slice(early, columns))[part]
            here = halo_in.at[:, cols]
            remote(here, here, sem_halo.at[part], sem_halo.at[2 + part], (me, 1 - core)).wait_recv()

    @pl.when(jnp.logical_not(has_down))
    def _():
        halo_in[...] = jnp.zeros_like(halo_in)

    tiles = all_rows // tile
    slots = (2 * planes - 2) * GROUP

    def late_slot(slot):
        q, below = plane_of(slot // GROUP + 1)

        @pl.when((q >= 0) & (q < planes))
        def _():
            relay_one(2, q, below, slot % GROUP)

    def column_step(j, carry):
        taps[0:8, :] = halo_in[:, wide(j)].astype(jnp.float32)[halo_rows - 8 :, :]

        def row_step(m, inner):
            rows = pl.ds(pl.multiple_of(m * tile, tile), tile)
            raw = jnp.dot(tok[rows, :], up_all[:, wide(j)], preferred_element_type=jnp.float32)
            taps[8:, :] = (raw * par[0:1, wide(j)]).astype(jnp.bfloat16).astype(jnp.float32)
            conv = par[4:5, wide(j)] + par[3:4, wide(j)] * taps[8 : 8 + tile, :]
            conv = conv + par[2:3, wide(j)] * taps[7 : 7 + tile, :]
            conv = conv + par[1:2, wide(j)] * taps[6 : 6 + tile, :]
            g, v = conv[:, :128], conv[:, 128:]
            act = 0.5 * g * (1.0 + jnp.tanh(math.sqrt(2.0 / math.pi) * (g + 0.044715 * (g * g * g))))
            hidden[rows, pl.ds(pl.multiple_of(j * 128, 128), 128)] = (act * v).astype(jnp.bfloat16)
            taps[0:8, :] = taps[tile : tile + 8, :]
            slot = j * tiles + m

            @pl.when((slot < slots) & (j < early // 256))
            def _():
                late_slot(slot)

            return inner

        return lax.fori_loop(0, tiles, row_step, carry)

    early_blocks = early // 256
    halo_part(0, 0, early_blocks)
    lax.fori_loop(0, early_blocks, column_step, 0)

    def late_rest(slot, carry):
        late_slot(slot)
        return carry

    if early_blocks * tiles < slots:
        lax.fori_loop(early_blocks * tiles, slots, late_rest, 0)
    for direction in (0, 1):
        forward(1, direction, me)
    own_plane(1)
    if early_blocks < blocks:
        halo_part(1, early_blocks, blocks)
        lax.fori_loop(early_blocks, blocks, column_step, 0)

    def block_rows(owner):
        return pl.ds(pl.multiple_of(owner * rows_own, rows_own), rows_own)

    def pair_copy(q, owner):
        return remote(
            stage.at[q, owner],
            pair_in.at[q % half, owner],
            sem_pair_send.at[q % half, owner],
            sem_pair_recv.at[q % half, owner],
            (me, 1 - core),
        )

    half_rows = rows_own // 2

    def half_of(which):
        return pl.ds(which * half_rows, half_rows)

    def peer_copy(q, mask, which):
        slot = (mask - 1) * 2 + which
        return remote(
            stage.at[q, flip(mask), half_of(which)],
            peer_in.at[q % half, mask - 1, half_of(which)],
            sem_peer_send.at[q % half, slot],
            sem_peer_recv.at[q % half, slot],
            chip(flip(mask)),
        )

    def relay_copy(q, mask):
        return remote(
            stage.at[q, flip(3), half_of(mask - 1)],
            relay_in.at[q % half, mask - 1],
            sem_relay_send.at[q % half, mask - 1],
            sem_relay_recv.at[q % half, mask - 1],
            chip(flip(mask)),
        )

    def down_step(step, carry):
        q, below = plane_of(step)

        @pl.when((q >= 0) & (q < planes))
        def _():
            @pl.when(step > 0)
            def _():
                relay(1, q, below)

            mine = q // half == core
            cols = pl.ds(pl.multiple_of(q * chunk, chunk), chunk)

            def product(owner, inner):
                value = jnp.dot(hidden[block_rows(owner), :], down_all[:, cols], preferred_element_type=jnp.float32)
                stage[q, owner] = value.astype(jnp.bfloat16)

                @pl.when(jnp.logical_not(mine))
                def _():
                    pair_copy(q, owner).start()

                return inner

            lax.fori_loop(0, GROUP, product, 0)

            @pl.when(mine)
            def _():
                def combine(owner):
                    pair_copy(q, owner).wait_recv()
                    both = stage[q, owner].astype(jnp.float32) + pair_in[q % half, owner].astype(jnp.float32)
                    stage[q, owner] = both.astype(jnp.bfloat16)

                combine(flip(3))
                for mask in (1, 2):
                    relay_copy(q, mask).start()
                for mask in (1, 2):
                    combine(flip(mask))
                    peer_copy(q, mask, mask - 1).start()
                combine(p)
                for mask in (1, 2):
                    relay_copy(q, mask).wait_recv()
                    owner = flip(3 - mask)
                    rows = half_of(mask - 1)
                    total = stage[q, owner, rows, :].astype(jnp.float32) + relay_in[q % half, mask - 1].astype(jnp.float32)
                    stage[q, owner, rows, :] = total.astype(jnp.bfloat16)
                    peer_copy(q, 3 - mask, mask - 1).start()

        return carry

    lax.fori_loop(0, 2 * planes - 1, down_step, 0)

    def finish(i, carry):
        q = core * half + i
        total = stage[q, p].astype(jnp.float32)
        for mask in (1, 2):
            for which in (0, 1):
                peer_copy(q, mask, which).wait_recv()
            total = total + peer_in[i, mask - 1].astype(jnp.float32)
        cols = pl.ds(pl.multiple_of(i * chunk, chunk), chunk)
        out[:, cols] = (total * osc[0:1, cols]).astype(jnp.bfloat16)
        return carry

    lax.fori_loop(0, half, finish, 0)

    def drain_out(i, carry):
        for mask in (1, 2):
            relay_copy(core * half + i, mask).wait_send()
            for which in (0, 1):
                peer_copy(core * half + i, mask, which).wait_send()

        def one(owner, inner):
            pair_copy((1 - core) * half + i, owner).wait_send()
            return inner

        return lax.fori_loop(0, GROUP, one, carry)

    lax.fori_loop(0, half, drain_out, 0)
    for mask in (1, 2):
        token_copy(mask).wait_send()
        token_relay(mask).wait_send()
    for mask in others:
        token_pair_copy(mask).wait_send()
        for kind in (0, 1, 2):
            plane_copy(kind, mask).wait_send()

    @pl.when(has_up)
    def _():
        halo_copy(0).wait_send()
        if early < columns:
            halo_copy(1).wait_send()

    def drain_line(f, carry):
        for kind in (0, 1, 2):

            @pl.when(has_up & (f // GROUP <= z))
            def _():
                line_copy(kind, 0, f).wait_send()

            @pl.when(has_down & (f // GROUP >= z))
            def _():
                line_copy(kind, 1, f).wait_send()

        return carry

    lax.fori_loop(0, planes * GROUP, drain_line, 0)


def grouped_body(count, tokens, norm_gain, gate_weight, value_weight, gate_scale, value_scale, gate_kernel, value_kernel, gate_bias, value_bias, down_weight, down_scale):
    planes = count // GROUP
    half = planes // 2
    rows, width = tokens.shape
    piece, local = gate_weight.shape
    out_piece = down_weight.shape[1]
    units = local // GROUP
    chunk = GROUP * out_piece
    tile = rows // 2
    dma = pltpu.SemaphoreType.DMA
    bf16, f32 = jnp.bfloat16, jnp.float32
    vmem = pl.BlockSpec(memory_space=pltpu.VMEM)
    hbm = pl.BlockSpec(memory_space=pl.ANY)
    return pl.pallas_call(
        functools.partial(fused_kernel, planes),
        out_shape=jax.ShapeDtypeStruct((rows, half * chunk), bf16),
        in_specs=[hbm] * 4 + [vmem] * 8,
        out_specs=vmem,
        scratch_shapes=[
            pltpu.VMEM((GROUP * rows, width), bf16),
            pltpu.VMEM((width, 2 * units), bf16),
            pltpu.VMEM((units, width), bf16),
            pltpu.VMEM((GROUP * rows, units), bf16),
            pltpu.VMEM((planes, GROUP, rows, chunk), bf16),
            pltpu.VMEM((half, GROUP, rows, chunk), bf16),
            pltpu.VMEM((half, 2, rows, chunk), bf16),
            pltpu.VMEM((half, 2, rows // 2, chunk), bf16),
            pltpu.VMEM((tile + 8, 256), f32),
            pltpu.VMEM((16, 2 * units), bf16),
            pltpu.VMEM((16, 2 * units), bf16),
            pltpu.VMEM((8, 2 * units), f32),
            pltpu.VMEM((GROUP, piece, 2 * units), bf16),
            pltpu.VMEM((GROUP, units, out_piece), bf16),
            pltpu.VMEM((rows, width), bf16),
            pltpu.VMEM((piece, local), f32),
            pltpu.VMEM((piece, local), f32),
            pltpu.VMEM((local, out_piece), f32),
            dma((6,)),
            dma((3, GROUP)),
            dma((count,)),
            dma((count,)),
            dma((2, count)),
            dma((2, count)),
            dma((GROUP,)),
            dma((GROUP,)),
            dma((GROUP,)),
            dma((GROUP,)),
            dma((4,)),
            dma((half, GROUP)),
            dma((half, GROUP)),
            dma((half, 4)),
            dma((half, 4)),
            dma((half, 2)),
            dma((half, 2)),
            dma((count,)),
            dma((2, count)),
        ],
        compiler_params=pltpu.CompilerParams(
            collective_id=0, has_side_effects=True, vmem_limit_bytes=67043328
        ),
    )(
        tokens,
        gate_weight,
        value_weight,
        down_weight,
        norm_gain[None, :],
        gate_scale[None, :],
        value_scale[None, :],
        gate_kernel,
        value_kernel,
        gate_bias[None, :],
        value_bias[None, :],
        down_scale[None, :],
    )


def solution(mesh):
    count, tp = mesh.shape["fs"], mesh.shape["tp"]

    def whole(*arrays):
        local = arrays[2].shape[1]
        fits = tp == 2 and count % (2 * GROUP) == 0 and local % (GROUP * 128) == 0
        if fits:
            return grouped_body(count, *arrays)
        return body(*arrays)

    return jax.shard_map(
        whole,
        mesh=mesh,
        in_specs=(
            P("fs", None),
            P(),
            P("fs", "tp"),
            P("fs", "tp"),
            P("tp"),
            P("tp"),
            P(None, "tp"),
            P(None, "tp"),
            P("tp"),
            P("tp"),
            P("tp", "fs"),
            P("tp"),
        ),
        out_specs=P("fs", "tp"),
        check_vma=False,
    )
```

```python
import functools
import math

import jax
import jax.numpy as jnp
from jax import lax
from jax.experimental import pallas as pl
from jax.experimental.pallas import tpu as pltpu
from jax.sharding import PartitionSpec as P

epsilon = 1e-06


def from_behind(value, axis, steps):
    count = lax.axis_size(axis)
    leading, last = (max(0, -steps), min(count, count - steps))
    return lax.ppermute(value, axis, [(source, source + steps) for source in range(leading, last)])


def normalize(tokens, norm_gain):
    values = tokens.astype(jnp.float32)
    scaled = values * lax.rsqrt(jnp.mean(values * values, axis=1, keepdims=True) + epsilon)
    return (scaled * norm_gain[None, :]).astype(jnp.bfloat16)


def causal_mix(current, previous, kernel, tap_bias):
    row_count = current.shape[0]
    joined = jnp.concatenate([previous, current], axis=0).astype(jnp.float32)
    summed_taps = tap_bias[None, :] + kernel[2][None, :] * joined[2:]
    for back_by in (1, 2):
        summed_taps = (
            summed_taps
            + kernel[2 - back_by][None, :] * joined[2 - back_by : 2 - back_by + row_count]
        )
    return summed_taps


def body(
    tokens,
    norm_gain,
    gate_weight,
    value_weight,
    gate_scale,
    value_scale,
    gate_kernel,
    value_kernel,
    gate_bias,
    value_bias,
    down_weight,
    down_scale,
):
    normed = normalize(tokens, norm_gain)
    gate_low = gate_weight.astype(jnp.bfloat16)
    value_low = value_weight.astype(jnp.bfloat16)
    down_low = down_weight.astype(jnp.bfloat16)
    row_count = normed.shape[0]
    gate_full, value_full, down_full = (
        lax.all_gather(gate_low, "fs", axis=0, tiled=True),
        lax.all_gather(value_low, "fs", axis=0, tiled=True),
        lax.all_gather(down_low, "fs", axis=1, tiled=True),
    )
    gate_raw = jnp.dot(normed, gate_full, preferred_element_type=jnp.float32)
    value_raw = jnp.dot(normed, value_full, preferred_element_type=jnp.float32)
    gate_pre = (gate_raw * gate_scale[None, :]).astype(jnp.bfloat16)
    value_pre = (value_raw * value_scale[None, :]).astype(jnp.bfloat16)
    previous_gate, previous_value = from_behind(
        (gate_pre[row_count - 2 :], value_pre[row_count - 2 :]), "fs", 1
    )
    gate_conv = causal_mix(gate_pre, previous_gate, gate_kernel, gate_bias)
    value_conv = causal_mix(value_pre, previous_value, value_kernel, value_bias)
    hidden = (jax.nn.gelu(gate_conv, approximate=True) * value_conv).astype(jnp.bfloat16)
    partial_terms = jnp.dot(hidden, down_full, preferred_element_type=jnp.float32)
    summed = lax.psum_scatter(
        partial_terms.astype(jnp.bfloat16), "tp", scatter_dimension=1, tiled=True
    ).astype(jnp.float32)
    return (summed * down_scale[None, :]).astype(jnp.bfloat16)


MESH = pl.DeviceIdType.MESH
GROUP = 4


def fused_kernel(
    depth_planes,
    tok_hbm,
    gate_hbm,
    value_hbm,
    down_hbm,
    gain,
    gate_scale,
    value_scale,
    gate_kernel,
    value_kernel,
    gate_bias,
    value_bias,
    osc,
    out,
    tok,
    up_all,
    down_all,
    hidden,
    stage,
    pair_in,
    peer_in,
    relay_in,
    taps,
    halo_out,
    halo_in,
    par,
    wu,
    wd,
    raw_tok,
    raw_gate,
    raw_value,
    raw_down,
    sem_local,
    sem_plane_send,
    sem_up_recv,
    sem_down_recv,
    sem_up_send,
    sem_down_send,
    sem_tok_send,
    sem_tok_recv,
    sem_tok_pair_send,
    sem_tok_pair_recv,
    sem_halo,
    sem_pair_send,
    sem_pair_recv,
    sem_peer_send,
    sem_peer_recv,
    sem_relay_send,
    sem_relay_recv,
    sem_late_recv,
    sem_late_send,
):
    planes = depth_planes
    half = planes // 2
    me = lax.axis_index("fs")
    core = lax.axis_index("tp")
    z, p = me // GROUP, me % GROUP
    rows_own = raw_tok.shape[0]
    part_rows = rows_own // 2
    piece = wu.shape[1]
    units = hidden.shape[1]
    out_piece = wd.shape[2]
    chunk = GROUP * out_piece
    has_up, has_down = z < planes - 1, z > 0

    def flip(mask):
        px, py = p % 2, p // 2
        if mask & 1:
            px = 1 - px
        if mask & 2:
            py = 1 - py
        return py * 2 + px

    def chip(target):
        return (z * GROUP + target, core)

    others = (1, 2, 3)

    fetches = [
        pltpu.make_async_copy(src, dst, sem_local.at[2 + i])
        for i, (src, dst) in enumerate(
            ((gate_hbm, raw_gate), (value_hbm, raw_value), (down_hbm, raw_down), (tok_hbm, raw_tok))
        )
    ]
    for fetch in fetches:
        fetch.start()

    barrier = pltpu.get_barrier_semaphore()
    for mask in others:
        pl.semaphore_signal(barrier, inc=1, device_id=chip(flip(mask)), device_id_type=MESH)
    pl.semaphore_signal(barrier, inc=1, device_id=(me, 1 - core), device_id_type=MESH)

    @pl.when(has_up)
    def _():
        pl.semaphore_signal(barrier, inc=1, device_id=(me + GROUP, core), device_id_type=MESH)

    @pl.when(has_down)
    def _():
        pl.semaphore_signal(barrier, inc=1, device_id=(me - GROUP, core), device_id_type=MESH)

    blocks = units // 128
    fetches[0].wait()
    fetches[1].wait()
    for m in range(GROUP):
        for j in range(blocks):
            first = (m * blocks + j) * 128
            wu[m, :, j * 256 : j * 256 + 128] = raw_gate[:, first : first + 128].astype(jnp.bfloat16)
            wu[m, :, j * 256 + 128 : j * 256 + 256] = raw_value[:, first : first + 128].astype(jnp.bfloat16)
    fetches[2].wait()
    for m in range(GROUP):
        wd[m] = raw_down[m * units : (m + 1) * units, :].astype(jnp.bfloat16)
    for j in range(blocks):
        src = pl.ds(pl.multiple_of(p * units + j * 128, 128), 128)
        for side, (scale, kernel, tap_bias) in enumerate(
            ((gate_scale, gate_kernel, gate_bias), (value_scale, value_kernel, value_bias))
        ):
            dst = slice(j * 256 + side * 128, j * 256 + side * 128 + 128)
            par[0:1, dst] = scale[0:1, src]
            par[1:4, dst] = kernel[0:3, src]
            par[4:5, dst] = tap_bias[0:1, src]
    pl.semaphore_wait(barrier, 4 + has_up.astype(jnp.int32) + has_down.astype(jnp.int32))

    early = (blocks + 1) // 2 * 256
    columns = up_all.shape[1]

    def up_whole(f):
        return up_all.at[pl.ds(pl.multiple_of(f * piece, piece), piece), :]

    def up_block(f):
        return up_all.at[pl.ds(pl.multiple_of(f * piece, piece), piece), 0:early]

    def late_block(f):
        return up_all.at[pl.ds(pl.multiple_of(f * piece, piece), piece), early:columns]

    def down_block(f):
        return down_all.at[:, pl.ds(pl.multiple_of(f * out_piece, out_piece), out_piece)]

    kinds = (
        (up_block, sem_up_send, sem_up_recv),
        (down_block, sem_down_send, sem_down_recv),
        (late_block, sem_late_send, sem_late_recv),
    )

    def remote(src, dst, send, recv, device):
        return pltpu.make_async_remote_copy(
            src_ref=src, dst_ref=dst, send_sem=send, recv_sem=recv, device_id=device, device_id_type=MESH
        )

    def plane_copy(kind, mask):
        target = flip(mask)
        block, _, recv = kinds[kind]
        src = (wu.at[target, :, 0:early], wd.at[target], wu.at[target, :, early:columns])[kind]
        return remote(src, block(me), sem_plane_send.at[kind, mask], recv.at[me], chip(target))

    def line_copy(kind, direction, f):
        block, send, recv = kinds[kind]
        step = GROUP if direction == 0 else -GROUP
        return remote(block(f), block(f), send.at[direction, f], recv.at[f], (me + step, core))

    def wait_piece(kind, f):
        block, send, recv = kinds[kind]
        remote(block(f), block(f), send.at[0, f], recv.at[f], (me, 1 - core)).wait_recv()

    def forward(kind, direction, f):
        @pl.when(has_up if direction == 0 else has_down)
        def _():
            line_copy(kind, direction, f).start()

    def token_rows(owner, part):
        start = pl.multiple_of(owner * rows_own + part * part_rows, part_rows)
        return tok.at[pl.ds(start, part_rows), :]

    def token_copy(mask):
        here = token_rows(p, core)
        return remote(here, here, sem_tok_send.at[mask], sem_tok_recv.at[mask], chip(flip(mask)))

    quarter = part_rows // 2

    def token_quarter(owner, which):
        start = owner * rows_own + core * part_rows + which * quarter
        return tok.at[pl.ds(pl.multiple_of(start, quarter), quarter), :]

    def token_relay(mask):
        which = mask - 1
        slot = (3, 0)[which]
        here = token_quarter(flip(mask), which)
        return remote(here, here, sem_tok_send.at[slot], sem_tok_recv.at[slot], chip(flip(3 - mask)))

    def token_pair_copy(mask):
        here = token_rows(flip(mask), core)
        return remote(here, here, sem_tok_pair_send.at[mask], sem_tok_pair_recv.at[mask], (me, 1 - core))

    own_up = pltpu.make_async_copy(wu.at[p], up_whole(me), sem_local.at[0])
    own_down = pltpu.make_async_copy(wd.at[p], down_block(me), sem_local.at[1])
    own_up.start()
    own_down.start()
    for kind in (0, 2):
        for mask in others:
            plane_copy(kind, mask).start()
    own_up.wait()
    for direction in (0, 1):
        forward(0, direction, me)

    fetches[3].wait()
    norm_tile = 64

    def norm_step(i, carry):
        first = pl.multiple_of(i * norm_tile, norm_tile)
        values = raw_tok[pl.ds(first, norm_tile), :].astype(jnp.float32)
        scaled = values * lax.rsqrt(jnp.mean(values * values, axis=1, keepdims=True) + epsilon)
        rows = pl.ds(pl.multiple_of(p * rows_own + i * norm_tile, norm_tile), norm_tile)
        tok[rows, :] = (scaled * gain[...]).astype(jnp.bfloat16)
        return carry

    lax.fori_loop(0, rows_own // norm_tile, norm_step, 0)
    own_down.wait()

    def own_plane(kind):
        for mask in others:
            f = z * GROUP + flip(mask)
            wait_piece(kind, f)
            for direction in (0, 1):
                forward(kind, direction, f)

    own_plane(0)
    for mask in (1, 2):
        token_copy(mask).start()
    for mask in others:
        plane_copy(1, mask).start()
    for direction in (0, 1):
        forward(2, direction, me)
    own_plane(2)

    def plane_of(step):
        distance = (step + 1) // 2
        below = step % 2
        return z + distance * (1 - 2 * below), below

    def relay_one(kind, q, below, i):
        f = q * GROUP + i
        wait_piece(kind, f)

        @pl.when((below == 1) & has_up)
        def _():
            line_copy(kind, 0, f).start()

        @pl.when((below == 0) & has_down)
        def _():
            line_copy(kind, 1, f).start()

    def relay(kind, q, below):
        def one(i, carry):
            relay_one(kind, q, below, i)
            return carry

        lax.fori_loop(0, GROUP, one, 0)

    def up_step(step, carry):
        q, below = plane_of(step)

        @pl.when((q >= 0) & (q < planes))
        def _():
            relay(0, q, below)

        return carry

    lax.fori_loop(1, 2 * planes - 3, up_step, 0)

    def token_wait(mask):
        landed = token_rows(flip(mask), core)
        remote(landed, landed, sem_tok_send.at[mask], sem_tok_recv.at[mask], (me, 1 - core)).wait_recv()

    for mask in (1, 2):
        token_wait(mask)
        token_relay(mask).start()
        token_pair_copy(mask).start()

    lax.fori_loop(2 * planes - 3, 2 * planes - 1, up_step, 0)

    def token_pair_wait(mask):
        there = token_rows(flip(mask), 1 - core)
        remote(there, there, sem_tok_pair_send.at[mask], sem_tok_pair_recv.at[mask], (me, 1 - core)).wait_recv()

    for which in (0, 1):
        slot = (3, 0)[which]
        landed = token_quarter(flip(3), which)
        remote(landed, landed, sem_tok_send.at[slot], sem_tok_recv.at[slot], (me, 1 - core)).wait_recv()
    token_pair_copy(3).start()
    for mask in others:
        token_pair_wait(mask)

    all_rows = tok.shape[0]
    tile = taps.shape[0] - 8
    halo_rows = halo_out.shape[0]

    def wide(j):
        return pl.ds(pl.multiple_of(j * 256, 256), 256)

    def halo_step(j, carry):
        raw = jnp.dot(tok[all_rows - halo_rows :, :], up_all[:, wide(j)], preferred_element_type=jnp.float32)
        halo_out[:, wide(j)] = (raw * par[0:1, wide(j)]).astype(jnp.bfloat16)
        return carry

    def halo_copy(part):
        cols = (slice(0, early), slice(early, columns))[part]
        here, there = halo_out.at[:, cols], halo_in.at[:, cols]
        return remote(here, there, sem_halo.at[part], sem_halo.at[2 + part], (me + GROUP, core))

    def halo_part(part, first, last):
        lax.fori_loop(first, last, halo_step, 0)

        @pl.when(has_up)
        def _():
            halo_copy(part).start()

        @pl.when(has_down)
        def _():
            cols = (slice(0, early), slice(early, columns))[part]
            here = halo_in.at[:, cols]
            remote(here, here, sem_halo.at[part], sem_halo.at[2 + part], (me, 1 - core)).wait_recv()

    @pl.when(jnp.logical_not(has_down))
    def _():
        halo_in[...] = jnp.zeros_like(halo_in)

    tiles = all_rows // tile
    slots = (2 * planes - 2) * GROUP
    per_tile = -(-slots // (early // 256 * tiles))

    def late_slot(slot):
        q, below = plane_of(slot // GROUP + 1)

        @pl.when((q >= 0) & (q < planes))
        def _():
            relay_one(2, q, below, slot % GROUP)

    def column_step(j, carry):
        taps[0:8, :] = halo_in[:, wide(j)].astype(jnp.float32)[halo_rows - 8 :, :]

        def row_step(m, inner):
            rows = pl.ds(pl.multiple_of(m * tile, tile), tile)
            raw = jnp.dot(tok[rows, :], up_all[:, wide(j)], preferred_element_type=jnp.float32)
            taps[8:, :] = (raw * par[0:1, wide(j)]).astype(jnp.bfloat16).astype(jnp.float32)
            conv = par[4:5, wide(j)] + par[3:4, wide(j)] * taps[8 : 8 + tile, :]
            conv = conv + par[2:3, wide(j)] * taps[7 : 7 + tile, :]
            conv = conv + par[1:2, wide(j)] * taps[6 : 6 + tile, :]
            g, v = conv[:, :128], conv[:, 128:]
            act = 0.5 * g * (1.0 + jnp.tanh(math.sqrt(2.0 / math.pi) * (g + 0.044715 * (g * g * g))))
            hidden[rows, pl.ds(pl.multiple_of(j * 128, 128), 128)] = (act * v).astype(jnp.bfloat16)
            taps[0:8, :] = taps[tile : tile + 8, :]
            for k in range(per_tile):
                slot = (j * tiles + m) * per_tile + k

                @pl.when((slot < slots) & (j < early // 256))
                def _():
                    late_slot(slot)

            return inner

        return lax.fori_loop(0, tiles, row_step, carry)

    early_blocks = early // 256
    halo_part(0, 0, early_blocks)
    lax.fori_loop(0, early_blocks, column_step, 0)

    for direction in (0, 1):
        forward(1, direction, me)
    own_plane(1)
    if early_blocks < blocks:
        halo_part(1, early_blocks, blocks)
        lax.fori_loop(early_blocks, blocks, column_step, 0)

    def block_rows(owner):
        return pl.ds(pl.multiple_of(owner * rows_own, rows_own), rows_own)

    def pair_copy(q, owner):
        return remote(
            stage.at[q, owner],
            pair_in.at[q % half, owner],
            sem_pair_send.at[q % half, owner],
            sem_pair_recv.at[q % half, owner],
            (me, 1 - core),
        )

    half_rows = rows_own // 2

    def half_of(which):
        return pl.ds(which * half_rows, half_rows)

    def peer_copy(q, mask, which):
        slot = (mask - 1) * 2 + which
        return remote(
            stage.at[q, flip(mask), half_of(which)],
            peer_in.at[q % half, mask - 1, half_of(which)],
            sem_peer_send.at[q % half, slot],
            sem_peer_recv.at[q % half, slot],
            chip(flip(mask)),
        )

    def relay_copy(q, mask):
        return remote(
            stage.at[q, flip(3), half_of(mask - 1)],
            relay_in.at[q % half, mask - 1],
            sem_relay_send.at[q % half, mask - 1],
            sem_relay_recv.at[q % half, mask - 1],
            chip(flip(mask)),
        )

    def down_step(step, carry):
        q, below = plane_of(step)

        @pl.when((q >= 0) & (q < planes))
        def _():
            @pl.when(step > 0)
            def _():
                relay(1, q, below)

            mine = q // half == core
            cols = pl.ds(pl.multiple_of(q * chunk, chunk), chunk)

            def product(owner, inner):
                value = jnp.dot(hidden[block_rows(owner), :], down_all[:, cols], preferred_element_type=jnp.float32)
                stage[q, owner] = value.astype(jnp.bfloat16)

                @pl.when(jnp.logical_not(mine))
                def _():
                    pair_copy(q, owner).start()

                return inner

            lax.fori_loop(0, GROUP, product, 0)

            @pl.when(mine)
            def _():
                def combine(owner):
                    pair_copy(q, owner).wait_recv()
                    both = stage[q, owner].astype(jnp.float32) + pair_in[q % half, owner].astype(jnp.float32)
                    stage[q, owner] = both.astype(jnp.bfloat16)

                combine(flip(3))
                for mask in (1, 2):
                    relay_copy(q, mask).start()
                for mask in (1, 2):
                    combine(flip(mask))
                    peer_copy(q, mask, mask - 1).start()
                combine(p)
                for mask in (1, 2):
                    relay_copy(q, mask).wait_recv()
                    owner = flip(3 - mask)
                    rows = half_of(mask - 1)
                    total = stage[q, owner, rows, :].astype(jnp.float32) + relay_in[q % half, mask - 1].astype(jnp.float32)
                    stage[q, owner, rows, :] = total.astype(jnp.bfloat16)
                    peer_copy(q, 3 - mask, mask - 1).start()

        return carry

    lax.fori_loop(0, 2 * planes - 1, down_step, 0)

    def finish(i, carry):
        q = core * half + i
        total = stage[q, p].astype(jnp.float32)
        for mask in (1, 2):
            for which in (0, 1):
                peer_copy(q, mask, which).wait_recv()
            total = total + peer_in[i, mask - 1].astype(jnp.float32)
        cols = pl.ds(pl.multiple_of(i * chunk, chunk), chunk)
        out[:, cols] = (total * osc[0:1, cols]).astype(jnp.bfloat16)
        return carry

    lax.fori_loop(0, half, finish, 0)

    def drain_out(i, carry):
        for mask in (1, 2):
            relay_copy(core * half + i, mask).wait_send()
            for which in (0, 1):
                peer_copy(core * half + i, mask, which).wait_send()

        def one(owner, inner):
            pair_copy((1 - core) * half + i, owner).wait_send()
            return inner

        return lax.fori_loop(0, GROUP, one, carry)

    lax.fori_loop(0, half, drain_out, 0)
    for mask in (1, 2):
        token_copy(mask).wait_send()
        token_relay(mask).wait_send()
    for mask in others:
        token_pair_copy(mask).wait_send()
        for kind in (0, 1, 2):
            plane_copy(kind, mask).wait_send()

    @pl.when(has_up)
    def _():
        halo_copy(0).wait_send()
        if early < columns:
            halo_copy(1).wait_send()

    def drain_line(f, carry):
        for kind in (0, 1, 2):

            @pl.when(has_up & (f // GROUP <= z))
            def _():
                line_copy(kind, 0, f).wait_send()

            @pl.when(has_down & (f // GROUP >= z))
            def _():
                line_copy(kind, 1, f).wait_send()

        return carry

    lax.fori_loop(0, planes * GROUP, drain_line, 0)


def grouped_body(count, tokens, norm_gain, gate_weight, value_weight, gate_scale, value_scale, gate_kernel, value_kernel, gate_bias, value_bias, down_weight, down_scale):
    planes = count // GROUP
    half = planes // 2
    rows, width = tokens.shape
    piece, local = gate_weight.shape
    out_piece = down_weight.shape[1]
    units = local // GROUP
    chunk = GROUP * out_piece
    tile = rows
    dma = pltpu.SemaphoreType.DMA
    bf16, f32 = jnp.bfloat16, jnp.float32
    vmem = pl.BlockSpec(memory_space=pltpu.VMEM)
    hbm = pl.BlockSpec(memory_space=pl.ANY)
    return pl.pallas_call(
        functools.partial(fused_kernel, planes),
        out_shape=jax.ShapeDtypeStruct((rows, half * chunk), bf16),
        in_specs=[hbm] * 4 + [vmem] * 8,
        out_specs=vmem,
        scratch_shapes=[
            pltpu.VMEM((GROUP * rows, width), bf16),
            pltpu.VMEM((width, 2 * units), bf16),
            pltpu.VMEM((units, width), bf16),
            pltpu.VMEM((GROUP * rows, units), bf16),
            pltpu.VMEM((planes, GROUP, rows, chunk), bf16),
            pltpu.VMEM((half, GROUP, rows, chunk), bf16),
            pltpu.VMEM((half, 2, rows, chunk), bf16),
            pltpu.VMEM((half, 2, rows // 2, chunk), bf16),
            pltpu.VMEM((tile + 8, 256), f32),
            pltpu.VMEM((16, 2 * units), bf16),
            pltpu.VMEM((16, 2 * units), bf16),
            pltpu.VMEM((8, 2 * units), f32),
            pltpu.VMEM((GROUP, piece, 2 * units), bf16),
            pltpu.VMEM((GROUP, units, out_piece), bf16),
            pltpu.VMEM((rows, width), bf16),
            pltpu.VMEM((piece, local), f32),
            pltpu.VMEM((piece, local), f32),
            pltpu.VMEM((local, out_piece), f32),
            dma((6,)),
            dma((3, GROUP)),
            dma((count,)),
            dma((count,)),
            dma((2, count)),
            dma((2, count)),
            dma((GROUP,)),
            dma((GROUP,)),
            dma((GROUP,)),
            dma((GROUP,)),
            dma((4,)),
            dma((half, GROUP)),
            dma((half, GROUP)),
            dma((half, 4)),
            dma((half, 4)),
            dma((half, 2)),
            dma((half, 2)),
            dma((count,)),
            dma((2, count)),
        ],
        compiler_params=pltpu.CompilerParams(
            collective_id=0, has_side_effects=True, vmem_limit_bytes=67043328
        ),
    )(
        tokens,
        gate_weight,
        value_weight,
        down_weight,
        norm_gain[None, :],
        gate_scale[None, :],
        value_scale[None, :],
        gate_kernel,
        value_kernel,
        gate_bias[None, :],
        value_bias[None, :],
        down_scale[None, :],
    )


def solution(mesh):
    count, tp = mesh.shape["fs"], mesh.shape["tp"]

    def whole(*arrays):
        local = arrays[2].shape[1]
        fits = tp == 2 and count % (2 * GROUP) == 0 and local % (GROUP * 128) == 0
        if fits:
            return grouped_body(count, *arrays)
        return body(*arrays)

    return jax.shard_map(
        whole,
        mesh=mesh,
        in_specs=(
            P("fs", None),
            P(),
            P("fs", "tp"),
            P("fs", "tp"),
            P("tp"),
            P("tp"),
            P(None, "tp"),
            P(None, "tp"),
            P("tp"),
            P("tp"),
            P("tp", "fs"),
            P("tp"),
        ),
        out_specs=P("fs", "tp"),
        check_vma=False,
    )
```
